32 devices in a mesh: rep: 2 (over x), fs: 8 (over z, y), tp: 2 (over core).
Axes of the slice: x: 2, y: 2, z: 4, core: 2. Of those that a mesh axis runs over, the one named last changes fastest.
Arguments:
- tokens: bfloat16 [16384, 2048], P(('rep', 'fs')), may hold values from -6 to 6
- norm_mix: bfloat16 [2048], replicated, may hold values from 0.099609375 to 1.8984375
- w_unit: bfloat16 [2048, 1024], P('fs', 'tp'), may hold values from -0.125 to 0.125
- w_value: bfloat16 [2048, 1024], P('fs', 'tp'), may hold values from -0.125 to 0.125
- spatial: bfloat16 [4, 128, 128], replicated, may hold values from -0.52734375 to 0.52734375
- spatial_bias: bfloat16 [4, 128], replicated, may hold values from 0.099609375 to 1.8984375
- group_gain: bfloat16 [1024], replicated, may hold values from 0.099609375 to 1.8984375
- group_shift: bfloat16 [1024], replicated, may hold values from -3 to 3
- w_mix_out: bfloat16 [1024, 2048], P('tp', 'fs'), may hold values from -0.1875 to 0.1875
- norm_ffn: bfloat16 [2048], replicated, may hold values from 0.099609375 to 1.8984375
- w_gate: bfloat16 [2048, 2816], P('fs', 'tp'), may hold values from -0.125 to 0.125
- w_up: bfloat16 [2048, 2816], P('fs', 'tp'), may hold values from -0.125 to 0.125
- w_down: bfloat16 [2816, 2048], P('tp', 'fs'), may hold values from -0.109375 to 0.109375
Outputs:
- layer_out: bfloat16 [16384, 2048], P(('rep', 'fs', 'tp'))
The draws below stay inside these ranges and needn't reach their ends.
All inputs are finite; a program needn't handle non-finite values.
Results may differ from the reference program's by a relative error of at most 0.008.
Values may be sent and summed in bfloat16 or wider, within the bound.
A program may use at most 128 MiB of HBM per device.

```python
import jax
import jax.numpy as jnp
from jax import lax

D = 2048
FF = 2816
GROUPS = 4
SPATIAL_WIDTH = 1024
BLOCK = 128
TOK_DEV = 1024
TOKENS = 16384


def shard_levels(key, shape, cuts, smallest, high):
    level, own = 1.0, jax.random.fold_in(key, 6)
    for dim, shards_of in cuts:
        steps = jnp.exp(jax.random.uniform(jax.random.fold_in(own, dim), (shards_of,), jnp.float32, smallest / len(cuts), high / len(cuts)))
        level = level * jnp.repeat(steps, shape[dim] // shards_of).reshape([-1 if axis == dim else 1 for axis in range(len(shape))])
    return level


def gaussian(stream_key, shape, scale, bound, split=(), held_as=jnp.bfloat16):
    values = jax.random.normal(stream_key, shape, jnp.float32) * scale
    if len(split) > 0:
        values = shard_levels(stream_key, shape, split, -0.22, 0.18) * values
    return jnp.clip(values, min=-bound, max=bound).astype(held_as)


def setup_inputs(seed: int = 0) -> dict:
    keys = jax.random.split(jax.random.key(seed), 14)
    return {
        "tokens": gaussian(keys[0], (TOKENS, D), 1.0, 6.0, ((0, 16),)),
        "norm_mix": jnp.clip(1.0 + 0.18 * jax.random.normal(keys[1], (D,), jnp.float32), 0.099609375, 1.8984375).astype(jnp.bfloat16),
        "w_unit": gaussian(keys[2], (D, SPATIAL_WIDTH), D ** -0.5, 0.125, ((0, 8), (1, 2))),
        "w_value": gaussian(keys[3], (D, SPATIAL_WIDTH), D ** -0.5, 0.125, ((0, 8), (1, 2))),
        "spatial": gaussian(keys[4], (GROUPS, BLOCK, BLOCK), (BLOCK ** -0.5), 0.52734375),
        "spatial_bias": jnp.clip(1.0 + 0.18 * jax.random.normal(keys[5], (GROUPS, BLOCK), jnp.float32), 0.099609375, 1.8984375).astype(jnp.bfloat16),
        "group_gain": jnp.clip(1.0 + 0.18 * jax.random.normal(keys[6], (SPATIAL_WIDTH,), jnp.float32), 0.099609375, 1.8984375).astype(jnp.bfloat16),
        "group_shift": gaussian(keys[7], (SPATIAL_WIDTH,), 0.5, 3.0),
        "w_mix_out": gaussian(keys[8], (SPATIAL_WIDTH, D), SPATIAL_WIDTH ** -0.5, 0.1875, ((0, 2), (1, 8))),
        "norm_ffn": jnp.clip(1.0 + 0.18 * jax.random.normal(keys[9], (D,), jnp.float32), 0.099609375, 1.8984375).astype(jnp.bfloat16),
        "w_gate": gaussian(keys[10], (D, FF), D ** -0.5, 0.125, ((0, 8), (1, 2))),
        "w_up": gaussian(keys[11], (D, FF), D ** -0.5, 0.125, ((0, 8), (1, 2))),
        "w_down": gaussian(keys[12], (FF, D), FF ** -0.5, 0.109375, ((0, 2), (1, 8))),
    }


def rms_scale(values, gain):
    values = values.astype(jnp.float32)
    scale = lax.rsqrt(lax.optimization_barrier(jnp.mean(values * values, axis=-1, keepdims=True)) + 1e-06)
    return values * scale * gain.astype(jnp.float32)

def spatial_unit(unit_pre, value_pre, spatial, spatial_bias, group_gain, group_shift):
    count, width = value_pre.shape
    groups = spatial.shape[0]
    block = spatial.shape[1]
    active = jax.nn.gelu(value_pre, approximate=True).reshape(count, groups, width // groups)
    center = lax.optimization_barrier(jnp.mean(active, axis=-1, keepdims=True))
    spread = lax.optimization_barrier(jnp.mean(jnp.square(active - center), axis=-1, keepdims=True))
    normal = ((active - center) * lax.rsqrt(spread + 1e-06)).reshape(count, width)
    normal = normal * group_gain.astype(jnp.float32) + group_shift.astype(jnp.float32)
    grouped = normal.astype(jnp.bfloat16)
    causal = jnp.tril(jnp.ones((block, block), dtype=bool))
    weights = jnp.where(causal[None], spatial, jnp.zeros_like(spatial))
    tiles = grouped.reshape(count // block, block, groups, width // groups)
    mixed = jnp.einsum('gts,nsgd->ntgd', weights.astype(jnp.float32), tiles.astype(jnp.float32))
    mixed = mixed + spatial_bias.astype(jnp.float32).T[None, :, :, None]
    return jax.nn.gelu(unit_pre, approximate=True) * mixed.reshape(count, width)

def reference(tokens, norm_mix, w_unit, w_value, spatial, spatial_bias, group_gain, group_shift, w_mix_out, norm_ffn, w_gate, w_up, w_down):

    def one_sequence(rows):
        normed = rms_scale(rows, norm_mix).astype(jnp.bfloat16)
        unit_pre = jnp.dot(normed, w_unit, preferred_element_type=jnp.float32)
        value_pre = jnp.dot(normed, w_value, preferred_element_type=jnp.float32)
        gated = spatial_unit(unit_pre, value_pre, spatial, spatial_bias, group_gain, group_shift).astype(jnp.bfloat16)
        h_mid = (rows.astype(jnp.float32) + jnp.dot(gated, w_mix_out, preferred_element_type=jnp.float32)).astype(jnp.bfloat16)
        normed_mid = rms_scale(h_mid, norm_ffn).astype(jnp.bfloat16)
        gate = jnp.dot(normed_mid, w_gate, preferred_element_type=jnp.float32)
        up = jnp.dot(normed_mid, w_up, preferred_element_type=jnp.float32)
        hidden = (jax.nn.silu(gate) * up).astype(jnp.bfloat16)
        return (h_mid.astype(jnp.float32) + jnp.dot(hidden, w_down, preferred_element_type=jnp.float32)).astype(jnp.bfloat16)
    sequences = tokens.reshape(-1, TOK_DEV, tokens.shape[1])
    return lax.map(one_sequence, sequences).reshape(tokens.shape)
```

```python
import functools

import jax
import jax.numpy as jnp
from jax import lax
from jax.experimental import pallas as pl
from jax.experimental.pallas import tpu as pltpu
from jax.sharding import PartitionSpec as P


def rms_scale(values, gain):
    values = values.astype(jnp.float32)
    scale = lax.rsqrt(jnp.mean(values * values, axis=-1, keepdims=True) + 1e-06)
    return values * scale * gain.astype(jnp.float32)


def spatial_unit(unit_pre, value_pre, spatial, spatial_bias, group_gain, group_shift):
    count, width = value_pre.shape
    groups = spatial.shape[0]
    block = spatial.shape[1]
    active = jax.nn.gelu(value_pre, approximate=True).reshape(count, groups, width // groups)
    center = jnp.mean(active, axis=-1, keepdims=True)
    spread = jnp.mean(jnp.square(active - center), axis=-1, keepdims=True)
    normal = ((active - center) * lax.rsqrt(spread + 1e-06)).reshape(count, width)
    normal = normal * group_gain.astype(jnp.float32) + group_shift.astype(jnp.float32)
    grouped = normal.astype(jnp.bfloat16)
    causal = jnp.tril(jnp.ones((block, block), dtype=bool))
    weights = jnp.where(causal[None], spatial, jnp.zeros_like(spatial))
    tiles = grouped.reshape(count // block, block, groups, width // groups)
    mixed = jnp.einsum("gts,nsgd->ntgd", weights, tiles, preferred_element_type=jnp.float32)
    mixed = mixed + spatial_bias.astype(jnp.float32).T[None, :, :, None]
    return jax.nn.gelu(unit_pre, approximate=True) * mixed.reshape(count, width)


def place_kernel(deep, at_ref, own_ref, near_ref, far_ref, near_x_ref, far_x_ref, out_ref):
    slot = pl.program_id(0)
    plane = at_ref[2]
    same = lax.rem(slot, 2) == at_ref[1]
    own = jnp.logical_and(same, slot // 2 == at_ref[0])
    part = near_x_ref.shape[1]
    main = near_ref.shape[1]

    @pl.when(own)
    def _():
        out_ref[...] = own_ref[...]

    for is_near, main_ref, extra_ref in (
        (jnp.logical_and(same, jnp.logical_not(own)), near_ref, near_x_ref),
        (jnp.logical_not(same), far_ref, far_x_ref),
    ):

        @pl.when(jnp.logical_and(is_near, plane == 0))
        def _():
            out_ref[:main, :] = main_ref[0]
            out_ref[main:, :] = extra_ref[0]

        @pl.when(jnp.logical_and(is_near, plane == 1))
        def _():
            out_ref[:part, :] = extra_ref[0]
            out_ref[part:, :] = main_ref[0]


def place(own, near, far, near_x, far_x, at, axis):
    rows, columns = own.shape
    deep = near.shape[0]
    main, part = near.shape[1], near_x.shape[1]

    def step(slot, at_ref):
        return lax.rem(at_ref[0] - slot // 2 + deep, deep)

    if axis == 0:
        shape, where = (2 * deep * rows, columns), lambda slot, at_ref: (slot, 0)
    else:
        shape, where = (rows, 2 * deep * columns), lambda slot, at_ref: (0, slot)
    return pl.pallas_call(
        functools.partial(place_kernel, deep),
        out_shape=jax.ShapeDtypeStruct(shape, own.dtype),
        grid_spec=pltpu.PrefetchScalarGridSpec(
            num_scalar_prefetch=1,
            grid=(2 * deep,),
            in_specs=[
                pl.BlockSpec((rows, columns), lambda slot, at_ref: (0, 0)),
                pl.BlockSpec((1, main, columns), lambda slot, at_ref: (step(slot, at_ref), 0, 0)),
                pl.BlockSpec((1, main, columns), lambda slot, at_ref: (step(slot, at_ref), 0, 0)),
                pl.BlockSpec(
                    (1, part, columns),
                    lambda slot, at_ref: (jnp.maximum(step(slot, at_ref) - 1, 0), 0, 0),
                ),
                pl.BlockSpec((1, part, columns), lambda slot, at_ref: (step(slot, at_ref), 0, 0)),
            ],
            out_specs=pl.BlockSpec((rows, columns), where),
        ),
        cost_estimate=pl.CostEstimate(
            flops=2 * deep * rows * columns * 2000, bytes_accessed=8 * deep * rows * columns, transcendentals=0
        ),
        name="place",
    )(at, own, near, far, near_x, far_x)


def fetch(shard, axis):
    deep = lax.axis_size("fs") // 2
    index = lax.axis_index("fs")
    line, side, plane = index // 2, lax.rem(index, 2), lax.axis_index("rep")
    rows = shard.shape[0]
    part = rows * 3 // 8 // 16 * 16
    main = rows - part
    mine = lax.dynamic_slice_in_dim(shard, plane * part, main, 0)
    ups, downs = [mine], [mine]
    for step in range(1, deep):
        up = [(2 * z + y, 2 * z + 2 + y) for z in range(step - 1, deep - 1) for y in range(2)]
        down = [(2 * z + y, 2 * z - 2 + y) for z in range(1, deep - step + 1) for y in range(2)]
        ups.append(lax.ppermute(ups[-1], "fs", up))
        downs.append(lax.ppermute(downs[-1], "fs", down))
    near = jnp.stack(
        [mine] + [jnp.where(line >= step, ups[step], downs[deep - step]) for step in range(1, deep)]
    )
    across = [(2 * z + y, 2 * z + 1 - y) for z in range(deep) for y in range(2)]
    far = lax.ppermute(near, "fs", across)
    start = plane * (main - part)
    twins = [(0, 1), (1, 0)]
    near_x = lax.ppermute(lax.dynamic_slice_in_dim(near[1:], start, part, 1), "rep", twins)
    far_x = lax.ppermute(lax.dynamic_slice_in_dim(far, start, part, 1), "rep", twins)
    at = jnp.stack([line, side, plane]).astype(jnp.int32)
    columns = shard.shape[1]
    if axis == 1 and columns % 128:
        rows_form = place(shard, near, far, near_x, far_x, at, 0)
        return rows_form.reshape(-1, rows, columns).swapaxes(0, 1).reshape(rows, -1)
    return place(shard, near, far, near_x, far_x, at, axis)


def on_device(
    tokens,
    norm_mix,
    w_unit,
    w_value,
    spatial,
    spatial_bias,
    group_gain,
    group_shift,
    w_mix_out,
    norm_ffn,
    w_gate,
    w_up,
    w_down,
):
    count = tokens.shape[0]
    half = count // lax.axis_size("tp")
    position = lax.axis_index("tp")
    row_start = position * half
    local_width = w_unit.shape[1]
    group_count = spatial.shape[0] // lax.axis_size("tp")
    group_start = position * group_count
    cores = [(0, 1), (1, 0)]
    spatial_local = lax.dynamic_slice_in_dim(spatial, group_start, group_count, 0)
    bias_local = lax.dynamic_slice_in_dim(spatial_bias, group_start, group_count, 0)
    gain_local = lax.dynamic_slice_in_dim(group_gain, position * local_width, local_width, 0)
    shift_local = lax.dynamic_slice_in_dim(group_shift, position * local_width, local_width, 0)
    inputs_whole = fetch(jnp.concatenate([w_value, w_unit], axis=1), 0)
    out_mine = fetch(w_mix_out, 1)
    gate_whole = fetch(w_gate, 0)
    up_whole = fetch(w_up, 0)
    down_mine = fetch(w_down, 1)
    out_other = lax.ppermute(out_mine, "tp", cores)
    down_other = lax.ppermute(down_mine, "tp", cores)

    normed = rms_scale(tokens, norm_mix).astype(jnp.bfloat16)
    both = jnp.dot(normed, inputs_whole, preferred_element_type=jnp.float32)
    gated = spatial_unit(
        both[:, local_width:],
        both[:, :local_width],
        spatial_local,
        bias_local,
        gain_local,
        shift_local,
    ).astype(jnp.bfloat16)
    kept = lax.dynamic_slice_in_dim(gated, row_start, half, 0)
    sent = lax.dynamic_slice_in_dim(gated, half - row_start, half, 0)
    arrived = lax.ppermute(sent, "tp", cores)
    own_rows = lax.dynamic_slice_in_dim(tokens, row_start, half, 0)
    own_mid = (
        own_rows.astype(jnp.float32)
        + jnp.dot(kept, out_mine, preferred_element_type=jnp.float32)
        + jnp.dot(arrived, out_other, preferred_element_type=jnp.float32)
    ).astype(jnp.bfloat16)
    normed_own = rms_scale(own_mid, norm_ffn).astype(jnp.bfloat16)
    normed_mid = jnp.concatenate([normed_own, lax.ppermute(normed_own, "tp", cores)], axis=0)
    gate = jnp.dot(normed_mid, gate_whole, preferred_element_type=jnp.float32)
    up = jnp.dot(normed_mid, up_whole, preferred_element_type=jnp.float32)
    hidden = (jax.nn.silu(gate) * up).astype(jnp.bfloat16)
    hidden_arrived = lax.ppermute(hidden[half:], "tp", cores)
    summed_rows = jnp.dot(hidden[:half], down_mine, preferred_element_type=jnp.float32)
    summed_rows = summed_rows + jnp.dot(
        hidden_arrived, down_other, preferred_element_type=jnp.float32
    )
    return (own_mid.astype(jnp.float32) + summed_rows).astype(jnp.bfloat16)


def solution(mesh):
    placed = (
        P(("rep", "fs"), None),
        P(),
        P("fs", "tp"),
        P("fs", "tp"),
        P(),
        P(),
        P(),
        P(),
        P("tp", "fs"),
        P(),
        P("fs", "tp"),
        P("fs", "tp"),
        P("tp", "fs"),
    )
    return jax.shard_map(
        on_device,
        mesh=mesh,
        in_specs=placed,
        out_specs=P(("rep", "fs", "tp"), None),
        check_vma=False,
    )
```

```python
import functools

import jax
import jax.numpy as jnp
from jax import lax
from jax.experimental import pallas as pl
from jax.experimental.pallas import tpu as pltpu
from jax.sharding import PartitionSpec as P

MESH = pl.DeviceIdType.MESH


def rms_scale(values, gain):
    values = values.astype(jnp.float32)
    scale = lax.rsqrt(jnp.mean(values * values, axis=-1, keepdims=True) + 1e-06)
    return values * scale * gain.astype(jnp.float32)


def spatial_unit(unit_pre, value_pre, spatial, spatial_bias, group_gain, group_shift):
    count, width = value_pre.shape
    groups = spatial.shape[0]
    block = spatial.shape[1]
    active = jax.nn.gelu(value_pre, approximate=True).reshape(count, groups, width // groups)
    center = jnp.mean(active, axis=-1, keepdims=True)
    spread = jnp.mean(jnp.square(active - center), axis=-1, keepdims=True)
    normal = ((active - center) * lax.rsqrt(spread + 1e-06)).reshape(count, width)
    normal = normal * group_gain.astype(jnp.float32) + group_shift.astype(jnp.float32)
    grouped = normal.astype(jnp.bfloat16)
    causal = jnp.tril(jnp.ones((block, block), dtype=bool))
    weights = jnp.where(causal[None], spatial, jnp.zeros_like(spatial))
    tiles = grouped.reshape(count // block, block, groups, width // groups)
    mixed = jnp.einsum("gts,nsgd->ntgd", weights, tiles, preferred_element_type=jnp.float32)
    mixed = mixed + spatial_bias.astype(jnp.float32).T[None, :, :, None]
    return jax.nn.gelu(unit_pre, approximate=True) * mixed.reshape(count, width)


def gather_kernel(count, *refs):
    shards, wholes = refs[:count], refs[count : 2 * count]
    send, recv, kept = refs[2 * count :]
    deep = lax.axis_size("fs") // 2
    me, plane = lax.axis_index("fs"), lax.axis_index("rep")
    line, side = me // 2, lax.rem(me, 2)

    barrier = pltpu.get_barrier_semaphore()
    across, twin = {"fs": 2 * line + 1 - side}, {"rep": 1 - plane}
    along = [{"fs": 2 * lax.rem(line + step, deep) + side} for step in range(1, deep)]
    for peer in along + [across, twin]:
        pl.semaphore_signal(barrier, inc=1, device_id=peer, device_id_type=MESH)
    pl.semaphore_wait(barrier, deep + 1)

    def near(step):
        return 2 * lax.rem(line - step + deep, deep) + side

    def far(step):
        return 2 * lax.rem(line - step + deep, deep) + 1 - side

    rows = shards[0].shape[0]
    part = rows * 3 // 8 // 16 * 16
    main = rows - part
    held = pl.ds(pl.multiple_of(plane * part, 16), main)
    given = pl.ds(pl.multiple_of(plane * main, 16), part)
    taken = pl.ds(pl.multiple_of((1 - plane) * main, 16), part)

    def copy(which, number, source, target, peer):
        return pltpu.make_async_remote_copy(
            src_ref=source,
            dst_ref=target,
            send_sem=send.at[which, number],
            recv_sem=recv.at[which, number],
            device_id=peer,
            device_id_type=MESH,
        )

    started = []

    def start(which, number, source, target, peer):
        one = copy(which, number, source, target, peer)
        one.start()
        started.append(one)

    def arrive(which, number, block, peer):
        copy(which, number, block, block, peer).wait_recv()

    own = []
    for which, (shard, whole) in enumerate(zip(shards, wholes)):
        for step in range(1, deep):
            start(which, step - 1, shard.at[held], whole.at[me, held], along[step - 1])
        start(which, deep - 1, shard.at[held], whole.at[me, held], across)
        own.append(pltpu.make_async_copy(shard, whole.at[me], kept.at[which]))
        own[-1].start()
    for which, whole in enumerate(wholes):
        for step in range(deep):
            if step:
                block = whole.at[near(step), held]
                arrive(which, step - 1, block, along[step - 1])
                start(which, deep - 1 + step, block, block, across)
                block = whole.at[near(step), given]
                start(which, 2 * deep - 2 + step, block, block, twin)
            if step:
                arrive(which, deep - 2 + step, whole.at[far(step - 1), held], across)
                block = whole.at[far(step - 1), given]
                start(which, 3 * deep - 3 + step, block, block, twin)
        arrive(which, 2 * deep - 2, whole.at[far(deep - 1), held], across)
        block = whole.at[far(deep - 1), given]
        start(which, 4 * deep - 3, block, block, twin)
    for which, whole in enumerate(wholes):
        for step in range(1, deep):
            arrive(which, 2 * deep - 2 + step, whole.at[near(step), taken], twin)
        for step in range(deep):
            arrive(which, 3 * deep - 2 + step, whole.at[far(step), taken], twin)
        own[which].wait()
    for one in started:
        one.wait_send()


def gather(shards, number):
    fs, count = lax.axis_size("fs"), len(shards)
    rows, columns = shards[0].shape
    wholes = pl.pallas_call(
        functools.partial(gather_kernel, count),
        out_shape=[jax.ShapeDtypeStruct((fs, rows, columns), shards[0].dtype)] * count,
        in_specs=[pl.BlockSpec(memory_space=pltpu.VMEM)] * count,
        out_specs=[pl.BlockSpec(memory_space=pl.ANY)] * count,
        scratch_shapes=[
            pltpu.SemaphoreType.DMA((count, 2 * fs - 2)),
            pltpu.SemaphoreType.DMA((count, 2 * fs - 2)),
            pltpu.SemaphoreType.DMA((count,)),
        ],
        compiler_params=pltpu.CompilerParams(collective_id=number, has_side_effects=True),
        cost_estimate=pl.CostEstimate(
            flops=count * fs * rows * columns * 10000,
            bytes_accessed=2 * count * fs * rows * columns,
            transcendentals=0,
        ),
        name="gather",
    )(*shards)
    return [whole.reshape(fs * rows, columns) for whole in wholes]


def on_device(
    tokens,
    norm_mix,
    w_unit,
    w_value,
    spatial,
    spatial_bias,
    group_gain,
    group_shift,
    w_mix_out,
    norm_ffn,
    w_gate,
    w_up,
    w_down,
):
    count = tokens.shape[0]
    half = count // lax.axis_size("tp")
    position = lax.axis_index("tp")
    row_start = position * half
    local_width = w_unit.shape[1]
    group_count = spatial.shape[0] // lax.axis_size("tp")
    group_start = position * group_count
    cores = [(0, 1), (1, 0)]
    spatial_local = lax.dynamic_slice_in_dim(spatial, group_start, group_count, 0)
    bias_local = lax.dynamic_slice_in_dim(spatial_bias, group_start, group_count, 0)
    gain_local = lax.dynamic_slice_in_dim(group_gain, position * local_width, local_width, 0)
    shift_local = lax.dynamic_slice_in_dim(group_shift, position * local_width, local_width, 0)
    value_whole, unit_whole = gather((w_value, w_unit), 0)
    out_mine = lax.all_gather(w_mix_out, "fs", axis=1, tiled=True)
    down_mine = lax.all_gather(w_down, "fs", axis=1, tiled=True)
    out_other = lax.ppermute(out_mine, "tp", cores)
    down_other = lax.ppermute(down_mine, "tp", cores)

    normed = rms_scale(tokens, norm_mix).astype(jnp.bfloat16)
    value_pre = jnp.dot(normed, value_whole, preferred_element_type=jnp.float32)
    unit_pre = jnp.dot(normed, unit_whole, preferred_element_type=jnp.float32)
    gated = spatial_unit(
        unit_pre, value_pre, spatial_local, bias_local, gain_local, shift_local
    ).astype(jnp.bfloat16)
    gated, w_gate, w_up = lax.optimization_barrier((gated, w_gate, w_up))
    gate_whole, up_whole = gather((w_gate, w_up), 1)
    kept = lax.dynamic_slice_in_dim(gated, row_start, half, 0)
    sent = lax.dynamic_slice_in_dim(gated, half - row_start, half, 0)
    arrived = lax.ppermute(sent, "tp", cores)
    own_rows = lax.dynamic_slice_in_dim(tokens, row_start, half, 0)
    own_mid = (
        own_rows.astype(jnp.float32)
        + jnp.dot(kept, out_mine, preferred_element_type=jnp.float32)
        + jnp.dot(arrived, out_other, preferred_element_type=jnp.float32)
    ).astype(jnp.bfloat16)
    normed_own = rms_scale(own_mid, norm_ffn).astype(jnp.bfloat16)
    normed_mid = jnp.concatenate([normed_own, lax.ppermute(normed_own, "tp", cores)], axis=0)
    gate = jnp.dot(normed_mid, gate_whole, preferred_element_type=jnp.float32)
    up = jnp.dot(normed_mid, up_whole, preferred_element_type=jnp.float32)
    hidden = (jax.nn.silu(gate) * up).astype(jnp.bfloat16)
    hidden_arrived = lax.ppermute(hidden[half:], "tp", cores)
    summed_rows = jnp.dot(hidden[:half], down_mine, preferred_element_type=jnp.float32)
    summed_rows = summed_rows + jnp.dot(
        hidden_arrived, down_other, preferred_element_type=jnp.float32
    )
    return (own_mid.astype(jnp.float32) + summed_rows).astype(jnp.bfloat16)


def solution(mesh):
    placed = (
        P(("rep", "fs"), None),
        P(),
        P("fs", "tp"),
        P("fs", "tp"),
        P(),
        P(),
        P(),
        P(),
        P("tp", "fs"),
        P(),
        P("fs", "tp"),
        P("fs", "tp"),
        P("tp", "fs"),
    )
    return jax.shard_map(
        on_device,
        mesh=mesh,
        in_specs=placed,
        out_specs=P(("rep", "fs", "tp"), None),
        check_vma=False,
    )
```
